32 devices in a mesh: ep: 4 (over y, x), tp: 8 (over z, core).
Axes of the slice: x: 2, y: 2, z: 4, core: 2. Of those that a mesh axis runs over, the one named last changes fastest.
Arguments:
- tokens: bfloat16 [2048, 2048], P('ep', 'tp'), may hold values from -6 to 6
- norm_gain: float32 [2048], replicated, may hold values from 0.1 to 1.9
- norm_shift: float32 [2048], replicated, may hold values from -3 to 3
- expert_ids: int32 [2048, 6], P('ep'), may hold values from 0 to 31, all different within a row; in each aligned block of 64 rows (0 to 63, 64 to 127, ...) at most 24 rows name the same one
- affinity: float32 [2048, 6], P('ep'), may hold values from 0.05 to 1
- expert_gate: bfloat16 [32, 2048, 512], P(('ep', 'tp')), may hold values from -0.125 to 0.125
- expert_up: bfloat16 [32, 2048, 512], P(('ep', 'tp')), may hold values from -0.125 to 0.125
- expert_down: bfloat16 [32, 512, 2048], P(('ep', 'tp')), may hold values from -0.25 to 0.25
- shared_gate: bfloat16 [512, 2048], P('tp'), may hold values from -0.125 to 0.125
- shared_up: bfloat16 [512, 2048], P('tp'), may hold values from -0.125 to 0.125
- shared_down: bfloat16 [512, 2048], replicated, may hold values from -0.25 to 0.25
Outputs:
- mixed: bfloat16 [2048, 2048], P(('ep', 'tp'))
The draws below stay inside these ranges and needn't reach their ends.
Inputs may be any that keep to these rules, and one draw needn't show every extreme that they name: `expert_ids`: each row names 6 different experts; in each aligned block of 64 rows (the rows of one device of tp) no expert is named more than 24 times, and in some blocks an expert is named exactly 24 times.
All inputs are finite; a program needn't handle non-finite values.
Results may differ from the reference program's by a relative error of at most 0.0069.
Values may be sent and summed in bfloat16 or wider, within the bound.
A program may use at most 64 MiB of HBM per device.

```python
import math
import jax
import jax.numpy as jnp
import numpy as np
from jax import lax

D = 2048
HID = 512
SHARED_HID = 512
TOP_K = 6
EXPERTS = 32
ROWS_BLK = 64
SLOTS = 24
TOKENS = 2048


def block_scale(stream_key, extent, cuts, least, top_value):
    level = 1.0
    for dim, parts in cuts:
        heights = jax.random.uniform(jax.random.fold_in(jax.random.fold_in(stream_key, 6), dim), (parts,), jnp.float32, least / len(cuts), top_value / len(cuts))
        level = level * jnp.repeat(jnp.exp(heights), extent[dim] // parts).reshape((-1,) + (1,) * (len(extent) - 1 - dim))
    return level


def routed_block(key, own, number, rows, number_of, top, bound, slope):
    ranking = jax.random.permutation(key, number_of)
    crowded, ordinary = portions_of(number_of, rows * top, bound, slope, True), portions_of(number_of, rows * top, bound, slope, False)
    places = jnp.arange(number_of)

    def named(lengths, rotation):
        used = int((lengths > 0).sum())
        fixed = max(1, used // 4)
        shifted = fixed + (places - fixed + rotation * (used - fixed)) % max(1, number_of - fixed)
        return jnp.zeros((number_of,), jnp.int32).at[ranking[jnp.where(places < fixed, places, shifted)]].set(jnp.asarray(lengths, jnp.int32))

    lengths = jnp.where(number % 4 == 0, named(crowded, number // 4), named(ordinary, number - number // 4 - 1))
    mixed = jax.random.permutation(jax.random.fold_in(own, 3), number_of)
    giver, sink = mixed[0:number_of // 2 * 2:2], mixed[1:number_of // 2 * 2:2]
    room = jnp.minimum(lengths[giver] - 1, bound - lengths[sink]) // 2
    room = jnp.where((giver == ranking[0]) | (sink == ranking[0]) | (lengths[sink] == 0), 0, jnp.maximum(room, 0))
    shifted = jax.random.randint(jax.random.fold_in(own, 4), (number_of // 2,), 0, 1 << 20) % (room + 1)
    lengths = lengths.at[giver].add(-shifted).at[sink].add(shifted)
    members = jnp.searchsorted(jnp.cumsum(lengths), jnp.arange(rows * top), side="right").astype(jnp.int32)
    listing = members.reshape(top, rows).T
    listing = listing[jax.random.permutation(jax.random.fold_in(own, 1), rows)]
    rotation = jax.random.randint(jax.random.fold_in(own, 2), (rows, 1), 0, top)
    return jnp.take_along_axis(listing, (jnp.arange(top)[None, :] + rotation) % top, axis=1)


def portions_of(count, total, reach, skew, full):
    portions = [(1 << 20) // math.isqrt(standing ** skew) + 1 for standing in range(1, count + 1)]
    largest = reach if full else min(reach, max(-(-total // count), total * portions[0] // sum(portions)))
    least = 1 if total - largest >= count - 1 else 0
    given, surplus = [largest] + [least] * (count - 1), total - largest - least * (count - 1)
    while surplus > 0:
        free = [i for i in range(1, count) if given[i] < largest] or [i for i in range(1, count) if given[i] < reach]
        pool, remaining = sum([portions[i] for i in free]), surplus
        for i in free:
            more = min(reach - given[i], max(1, remaining * portions[i] // pool), surplus)
            given[i] = given[i] + more
            surplus = surplus - more
    return np.array(given)


def normal_values(rng, extent, width, most, cuts=(), kind=jnp.bfloat16):
    entries = width * jax.random.normal(rng, extent, jnp.float32)
    if cuts:
        entries = entries * block_scale(rng, extent, cuts, -0.22, 0.18)
    return jnp.clip(entries, -most, most).astype(kind)


def setup_inputs(seed: int = 0) -> dict:
    key_of = jax.random.split(jax.random.key(seed), 12)
    tokens = normal_values(key_of[0], (TOKENS, D), 1.0, 6.0, ((0, 4), (1, 8)))
    norm_gain = jnp.clip(1.0 + 0.18 * jax.random.normal(key_of[1], (D,), jnp.float32), 0.1, 1.9)
    norm_shift = normal_values(key_of[2], (D,), 0.5, 3.0, (), jnp.float32)
    expert_ids_keys = jax.random.split(jax.random.fold_in(key_of[3], 1), TOKENS // ROWS_BLK)
    expert_ids_turns = jax.random.permutation(jax.random.fold_in(key_of[3], 3), TOKENS // ROWS_BLK)
    expert_ids = jax.vmap(lambda own, number: routed_block(jax.random.fold_in(key_of[3], 2), own, number, ROWS_BLK, EXPERTS, TOP_K, SLOTS, 2))(expert_ids_keys, expert_ids_turns).reshape((TOKENS, TOP_K))
    affinity = jnp.clip(0.05 + 0.95 * jax.random.uniform(key_of[4], (TOKENS, TOP_K), jnp.float32) ** block_scale(key_of[4], (TOKENS, TOP_K), ((0, 4),), -0.2, 0.2), 0.05, 1.0)
    expert_gate = normal_values(key_of[5], (EXPERTS, D, HID), D ** -0.5, 0.125, ((0, 32),))
    expert_up = normal_values(key_of[6], (EXPERTS, D, HID), D ** -0.5, 0.125, ((0, 32),))
    expert_down = normal_values(key_of[7], (EXPERTS, HID, D), HID ** -0.5, 0.25, ((0, 32),))
    shared_gate = normal_values(key_of[8], (SHARED_HID, D), D ** -0.5, 0.125, ((0, 8),))
    shared_up = normal_values(key_of[9], (SHARED_HID, D), D ** -0.5, 0.125, ((0, 8),))
    shared_down = normal_values(key_of[10], (SHARED_HID, D), SHARED_HID ** -0.5, 0.25)
    return dict(tokens=tokens, norm_gain=norm_gain, norm_shift=norm_shift, expert_ids=expert_ids, affinity=affinity, expert_gate=expert_gate, expert_up=expert_up, expert_down=expert_down, shared_gate=shared_gate, shared_up=shared_up, shared_down=shared_down)


ROUTED_SCALE = 2.5
EPSILON = 1e-05

def pair_ranks(flat_ids, expert_count):
    onehot = flat_ids[..., None] == jnp.arange(expert_count, dtype=jnp.int32)
    running = jnp.cumsum(onehot.astype(jnp.int32), axis=-2)
    return (lax.optimization_barrier(jnp.sum(jnp.where(onehot, running, 0), axis=-1)) - 1).astype(jnp.int32)

def expert_rows(tok_rows, w_gate, w_up, w_down):
    gate_act = jnp.dot(tok_rows, w_gate, preferred_element_type=jnp.float32)
    up_act = jnp.dot(tok_rows, w_up, preferred_element_type=jnp.float32)
    hidden = (jax.nn.silu(gate_act) * up_act).astype(jnp.bfloat16)
    return jnp.dot(hidden, w_down, preferred_element_type=jnp.float32).astype(jnp.bfloat16)

def rank_block(block_ids):
    return pair_ranks(block_ids, EXPERTS)

def reference(tokens, norm_gain, norm_shift, expert_ids, affinity, expert_gate, expert_up, expert_down, shared_gate, shared_up, shared_down):
    values = tokens.astype(jnp.float32)
    center = values - lax.optimization_barrier(jnp.mean(values, axis=1, keepdims=True))
    spread = lax.optimization_barrier(jnp.mean(center * center, axis=1, keepdims=True))
    normed = (center * lax.rsqrt(spread + EPSILON) * norm_gain + norm_shift).astype(jnp.bfloat16)
    weights = affinity / lax.optimization_barrier(jnp.sum(affinity, axis=1, keepdims=True)) * ROUTED_SCALE
    contract = (((1,), (1,)), ((), ()))
    shared_g = lax.dot_general(normed, shared_gate, contract, preferred_element_type=jnp.float32)
    shared_u = lax.dot_general(normed, shared_up, contract, preferred_element_type=jnp.float32)
    shared_hidden = (jax.nn.silu(shared_g) * shared_u).astype(jnp.bfloat16)
    shared_out = jnp.dot(shared_hidden, shared_down, preferred_element_type=jnp.float32)
    blocks = TOKENS // ROWS_BLK
    block_ids = expert_ids.reshape(blocks, ROWS_BLK * TOP_K).astype(jnp.int32)
    ranks = lax.map(rank_block, block_ids)
    block_index = jnp.arange(blocks, dtype=jnp.int32)[:, None]
    dest = (block_ids * blocks + block_index) * SLOTS + ranks
    token_index = block_index * ROWS_BLK + jnp.arange(ROWS_BLK * TOP_K, dtype=jnp.int32)[None, :] // TOP_K
    token_index = jnp.broadcast_to(token_index, dest.shape)
    per_expert = blocks * SLOTS
    source_row = jnp.full((EXPERTS * per_expert,), TOKENS, jnp.int32).at[dest.reshape(-1)].set(token_index.reshape(-1))
    source_row = source_row.reshape(EXPERTS, per_expert)
    slot_weight = jnp.zeros((EXPERTS * per_expert,), jnp.float32).at[dest.reshape(-1)].set(weights.reshape(-1))
    slot_weight = slot_weight.reshape(EXPERTS, per_expert)

    def one_expert(total, inputs):
        w_gate, w_up, w_down, row_index, row_weight = inputs
        tok_rows = jnp.take(normed, row_index, axis=0, mode='fill', fill_value=0)
        result = expert_rows(tok_rows, w_gate, w_up, w_down)
        total = total.at[row_index].add(result.astype(jnp.float32) * row_weight[:, None], mode='drop')
        return (total, None)
    routed, unused = lax.scan(one_expert, jnp.zeros((TOKENS, D), jnp.float32), (expert_gate, expert_up, expert_down, source_row, slot_weight))
    return (routed + shared_out).astype(jnp.bfloat16)
```

```python
import jax
import jax.numpy as jnp
from jax import lax
from jax.sharding import PartitionSpec as P

ROUTED_SCALE = 2.5
EPSILON = 1e-05


def expert_rows(tok_rows, w_gate, w_up, w_down):
    gate_act = jnp.dot(tok_rows, w_gate, preferred_element_type=jnp.float32)
    up_act = jnp.dot(tok_rows, w_up, preferred_element_type=jnp.float32)
    hidden = (jax.nn.silu(gate_act) * up_act).astype(jnp.bfloat16)
    return jnp.dot(hidden, w_down, preferred_element_type=jnp.float32).astype(jnp.bfloat16)


def on_device(
    tokens,
    norm_gain,
    norm_shift,
    expert_ids,
    affinity,
    expert_gate,
    expert_up,
    expert_down,
    shared_gate,
    shared_up,
    shared_down,
):
    ep_count = lax.axis_size("ep")
    tp_count = lax.axis_size("tp")
    tp_index = lax.axis_index("tp")
    whole = lax.all_gather(tokens, "tp", axis=1, tiled=True)
    tok_count = whole.shape[0]
    width = whole.shape[1]
    top_count = expert_ids.shape[1]
    block_rows = tok_count // tp_count
    expert_count = ep_count * tp_count
    slot_cap = max(1, 2 * block_rows * top_count // expert_count)
    slot_total = expert_count * slot_cap
    values = whole.astype(jnp.float32)
    center = values - jnp.mean(values, axis=1, keepdims=True)
    spread = jnp.mean(center * center, axis=1, keepdims=True)
    normed = (center * lax.rsqrt(spread + EPSILON) * norm_gain + norm_shift).astype(jnp.bfloat16)
    weights = affinity / jnp.sum(affinity, axis=1, keepdims=True) * ROUTED_SCALE
    contract = (((1,), (1,)), ((), ()))
    shared_g = lax.dot_general(shared_gate, normed, contract, preferred_element_type=jnp.float32)
    shared_u = lax.dot_general(shared_up, normed, contract, preferred_element_type=jnp.float32)
    shared_hidden = (jax.nn.silu(shared_g) * shared_u).astype(jnp.bfloat16)
    down_part = lax.dynamic_slice_in_dim(
        shared_down, tp_index * shared_gate.shape[0], shared_gate.shape[0], axis=0
    )
    experts = jnp.arange(ep_count, dtype=jnp.int32) * tp_count + tp_index
    hits = expert_ids[:, None, :] == experts[None, :, None]
    chosen = jnp.any(hits, axis=2)
    pair_weight = jnp.sum(jnp.where(hits, weights[:, None, :], 0), axis=2)
    rows = jnp.arange(tok_count, dtype=jnp.int32)
    before = (rows[:, None] > rows[None, :]) & (
        rows[:, None] // block_rows == rows[None, :] // block_rows
    )
    ranks = jnp.dot(
        before.astype(jnp.bfloat16), chosen.astype(jnp.bfloat16), preferred_element_type=jnp.float32
    ).astype(jnp.int32)
    place = jnp.where(chosen, (rows // block_rows)[:, None] * slot_cap + ranks, -1)
    slots = jnp.arange(tp_count * slot_cap, dtype=jnp.int32)
    pick = (place.T[:, None, :] == slots[None, :, None]).astype(jnp.bfloat16)
    outgoing = jnp.dot(
        pick.reshape(slot_total, tok_count), normed, preferred_element_type=jnp.float32
    ).astype(jnp.bfloat16)
    outgoing = outgoing.reshape(ep_count, tp_count * slot_cap, width)
    incoming = lax.all_to_all(outgoing, "ep", split_axis=0, concat_axis=0, tiled=True)
    result = expert_rows(incoming.reshape(-1, width), expert_gate[0], expert_up[0], expert_down[0])
    returned = lax.all_to_all(
        result.reshape(incoming.shape), "ep", split_axis=0, concat_axis=0, tiled=True
    )
    spread_weight = jnp.where(
        place[:, :, None] == slots[None, None, :], pair_weight[:, :, None], 0
    ).reshape(tok_count, slot_total).astype(jnp.bfloat16)
    part = jnp.dot(
        spread_weight, returned.reshape(slot_total, width), preferred_element_type=jnp.float32
    ) + lax.dot_general(
        shared_hidden, down_part, (((0,), (0,)), ((), ())), preferred_element_type=jnp.float32
    )
    total = lax.psum_scatter(part.astype(jnp.bfloat16), "tp", scatter_dimension=0, tiled=True)
    return total.astype(jnp.bfloat16)


def solution(mesh):
    placed = (
        P("ep", "tp"),
        P(),
        P(),
        P("ep", None),
        P("ep", None),
        P(("ep", "tp"), None, None),
        P(("ep", "tp"), None, None),
        P(("ep", "tp"), None, None),
        P("tp", None),
        P("tp", None),
        P(),
    )
    return jax.shard_map(
        on_device, mesh=mesh, in_specs=placed, out_specs=P(("ep", "tp"), None), check_vma=False
    )
```

```python
import functools
import math

import jax
import jax.numpy as jnp
from jax import lax
from jax.experimental import pallas as pl
from jax.experimental.pallas import tpu as pltpu
from jax.sharding import PartitionSpec as P

ROUTED_SCALE = 2.5
EPSILON = 1e-05
MESH = pl.DeviceIdType.MESH
F32 = jnp.float32
BF16 = jnp.bfloat16


def layer_kernel(
    sizes,
    tokens_ref,
    slot_ref,
    slot_t_ref,
    weight_ref,
    gain_ref,
    shift_ref,
    sgate_ref,
    sup_ref,
    gate_hbm,
    up_hbm,
    down_hbm,
    sdown_hbm,
    out_ref,
    gate_ref,
    up_ref,
    down_ref,
    sdown_ref,
    whole,
    pick,
    spread,
    sent,
    inc,
    norm,
    hidden,
    shidden,
    res,
    ret,
    part,
    own,
    pair_out,
    pair_in,
    far_out,
    far_in,
    load_sem,
    a_send,
    f_send,
    a_recv,
    b_send,
    b_recv,
    r_send,
    r_recv,
    p_send,
    p_recv,
    q_send,
    q_recv,
):
    ep, tp, rows, slots, feat, chunks, cols = sizes
    chips = tp // 2
    g = lax.axis_index("ep")
    t = lax.axis_index("tp")
    z = t // 2
    c = t % 2
    mate = z * 2 + 1 - c
    width = tp * feat
    shared_rows = sdown_ref.shape[0]

    loads = [
        pltpu.make_async_copy(gate_hbm, gate_ref, load_sem.at[0]),
        pltpu.make_async_copy(up_hbm, up_ref, load_sem.at[1]),
        pltpu.make_async_copy(down_hbm, down_ref, load_sem.at[2]),
        pltpu.make_async_copy(
            sdown_hbm.at[pl.ds(pl.multiple_of(t * shared_rows, 8), shared_rows)],
            sdown_ref,
            load_sem.at[3],
        ),
    ]
    for load in loads:
        load.start()

    def remote(src, dst, send, recv, e, k):
        return pltpu.make_async_remote_copy(
            src_ref=src,
            dst_ref=dst,
            send_sem=send,
            recv_sem=recv,
            device_id=(e, k),
            device_id_type=MESH,
        )

    barrier = pltpu.get_barrier_semaphore()
    partners = [(lax.rem(g + p, ep), t) for p in range(1, ep)]
    partners += [(g, lax.rem(z + d, chips) * 2 + c) for d in range(1, chips)]
    partners += [(g, mate)]
    for e, k in partners:
        pl.semaphore_signal(barrier, inc=1, device_id=(e, k), device_id_type=MESH)
    pl.semaphore_wait(barrier, len(partners))

    first = []
    first.append(remote(tokens_ref, whole.at[t], f_send.at[0], a_recv.at[t], g, mate))
    for d in range(1, chips):
        there = lax.rem(z + d, chips) * 2 + c
        first.append(remote(tokens_ref, whole.at[t], a_send.at[d], a_recv.at[t], g, there))
    for copy in first:
        copy.start()
    whole[t] = tokens_ref[...]

    for e in range(ep):
        line = lax.broadcasted_iota(jnp.int32, (slots, rows), 0) + e * slots
        pick[e] = jnp.where(line == slot_t_ref[e : e + 1, :], 1.0, 0.0).astype(BF16)
    line = lax.broadcasted_iota(jnp.int32, (rows, ep * slots), 1)
    mixed = jnp.zeros((rows, ep * slots), F32)
    for e in range(ep):
        mixed = jnp.where(line == slot_ref[:, e : e + 1], weight_ref[:, e : e + 1], mixed)
    spread[...] = mixed.astype(BF16)

    def forward(k, d):
        return remote(whole.at[k], whole.at[k], f_send.at[d], a_recv.at[k], g, mate)

    def chunk_step(i, carry):
        d = i // 2
        side = i % 2
        zz = lax.rem(z + d, chips)
        k = zz * 2 + lax.rem(c + side, 2)

        @pl.when(i > 0)
        def _():
            forward(k, d).wait_recv()

        @pl.when((i > 0) & (side == 0))
        def _():
            forward(k, d).start()

        picked = jnp.dot(
            pick[...].reshape(ep * slots, rows), whole[k], preferred_element_type=F32
        ).astype(BF16)
        sent[k] = picked.reshape(ep, slots, feat)
        inc[k, g] = sent[k, g]
        for p in range(1, ep):
            e = lax.rem(g + p, ep)
            remote(
                sent.at[k, e], inc.at[k, g], b_send.at[k, e], b_recv.at[k, g], e, t
            ).start()
        return carry

    lax.fori_loop(0, tp, chunk_step, 0)

    def normalise(read, count):
        tile = math.gcd(64, count)

        def body(i, carry):
            at = pl.ds(pl.multiple_of(i * tile, tile), tile)
            total = jnp.zeros((tile, feat), F32)
            for k in range(tp):
                total = total + read(k, at).astype(F32)
            mean = jnp.sum(total, axis=1, keepdims=True) / width
            total = jnp.zeros((tile, feat), F32)
            for k in range(tp):
                center = read(k, at).astype(F32) - mean
                total = total + center * center
            scale = lax.rsqrt(jnp.sum(total, axis=1, keepdims=True) / width + EPSILON)
            for k in range(tp):
                lanes = slice(k * feat, (k + 1) * feat)
                value = (read(k, at).astype(F32) - mean) * scale
                value = value * gain_ref[:, lanes] + shift_ref[:, lanes]
                norm[at, lanes] = value.astype(BF16)
            return carry

        lax.fori_loop(0, count // tile, body, 0)

    normalise(lambda k, at: whole[k, at, :], rows)
    contract = (((1,), (1,)), ((), ()))
    sg = lax.dot_general(norm[...], sgate_ref[...], contract, preferred_element_type=F32)
    su = lax.dot_general(norm[...], sup_ref[...], contract, preferred_element_type=F32)
    shidden[...] = (jax.nn.silu(sg) * su).astype(BF16)

    for load in loads:
        load.wait()

    def expert_step(p, carry):
        s = lax.rem(g + p, ep)

        @pl.when(p > 0)
        def _():
            for k in range(tp):
                remote(
                    sent.at[k, s], inc.at[k, s], b_send.at[k, s], b_recv.at[k, s], s, t
                ).wait_recv()

        normalise(lambda k, at: inc[k, s, at, :], slots)
        got = norm[0:slots, :]
        gate_act = jnp.dot(got, gate_ref[...], preferred_element_type=F32)
        up_act = jnp.dot(got, up_ref[...], preferred_element_type=F32)
        hidden[s] = (jax.nn.silu(gate_act) * up_act).astype(BF16)
        return carry

    lax.fori_loop(0, ep, expert_step, 0)

    def lanes_of(i):
        return pl.ds(pl.multiple_of(i * cols, cols), cols)

    def down_step(i, carry):
        rows_out = jnp.dot(
            hidden[...].reshape(ep * slots, hidden.shape[2]),
            down_ref[:, lanes_of(i)],
            preferred_element_type=F32,
        ).astype(BF16)
        res[i] = rows_out.reshape(ep, slots, cols)
        ret[i, g] = res[i, g]
        for p in range(1, ep):
            e = lax.rem(g + p, ep)
            remote(
                res.at[i, e], ret.at[i, g], r_send.at[i, e], r_recv.at[i, g], e, t
            ).start()
        return carry

    lax.fori_loop(0, chunks, down_step, 0)

    def pair_copy(i):
        return remote(pair_out.at[i], pair_in.at[i], p_send.at[i], p_recv.at[i], g, mate)

    def sum_step(i, carry):
        for p in range(1, ep):
            s = lax.rem(g + p, ep)
            remote(
                res.at[i, s], ret.at[i, s], r_send.at[i, s], r_recv.at[i, s], s, t
            ).wait_recv()
        total = jnp.dot(
            spread[...], ret[i].reshape(ep * slots, cols), preferred_element_type=F32
        ) + jnp.dot(shidden[...], sdown_ref[:, lanes_of(i)], preferred_element_type=F32)
        part[...] = total.reshape(part.shape)
        for zz in range(chips):
            pair_out[i, zz] = part[zz * 2 + 1 - c].astype(BF16)
        pair_copy(i).start()
        pair_copy(i).wait_recv()
        own[i] = part[t] + pair_in[i, z].astype(F32)
        for d in range(1, chips):
            zz = lax.rem(z + d, chips)
            far_out[i, zz] = (part[zz * 2 + c] + pair_in[i, zz].astype(F32)).astype(BF16)
            remote(
                far_out.at[i, zz],
                far_in.at[i, z],
                q_send.at[i, zz],
                q_recv.at[i, z],
                g,
                zz * 2 + c,
            ).start()
        return carry

    lax.fori_loop(0, chunks, sum_step, 0)

    def out_step(i, carry):
        total = own[i]
        for d in range(1, chips):
            zz = lax.rem(z + d, chips)
            remote(
                far_out.at[i, zz],
                far_in.at[i, zz],
                q_send.at[i, zz],
                q_recv.at[i, zz],
                g,
                zz * 2 + c,
            ).wait()
            total = total + far_in[i, zz].astype(F32)
        out_ref[:, lanes_of(i)] = total.astype(BF16)
        pair_copy(i).wait_send()
        for p in range(1, ep):
            e = lax.rem(g + p, ep)
            remote(
                res.at[i, e], ret.at[i, e], r_send.at[i, e], r_recv.at[i, e], e, t
            ).wait_send()
        return carry

    lax.fori_loop(0, chunks, out_step, 0)

    for copy in first:
        copy.wait_send()
    for d in range(1, chips):
        k = lax.rem(z + d, chips) * 2 + c
        forward(k, d).wait_send()

    def drain(k, carry):
        for p in range(1, ep):
            e = lax.rem(g + p, ep)
            remote(
                sent.at[k, e], inc.at[k, e], b_send.at[k, e], b_recv.at[k, e], e, t
            ).wait_send()
        return carry

    lax.fori_loop(0, tp, drain, 0)


def on_device(
    tokens,
    norm_gain,
    norm_shift,
    expert_ids,
    affinity,
    expert_gate,
    expert_up,
    expert_down,
    shared_gate,
    shared_up,
    shared_down,
):
    ep = lax.axis_size("ep")
    tp = lax.axis_size("tp")
    tp_index = lax.axis_index("tp")
    rows, feat = tokens.shape
    width = feat * tp
    top_count = expert_ids.shape[1]
    block = rows // tp
    expert_count = ep * tp
    slot_cap = max(1, 2 * block * top_count // expert_count)
    slots = tp * slot_cap
    hid = expert_gate.shape[2]
    shared_rows = shared_gate.shape[0]
    cols = 256
    chunks = width // cols
    chips = tp // 2

    weights = affinity / jnp.sum(affinity, axis=1, keepdims=True) * ROUTED_SCALE
    experts = jnp.arange(ep, dtype=jnp.int32) * tp + tp_index
    hits = expert_ids[:, None, :] == experts[None, :, None]
    chosen = jnp.any(hits, axis=2)
    pair_weight = jnp.sum(jnp.where(hits, weights[:, None, :], 0), axis=2)
    order = jnp.arange(rows, dtype=jnp.int32)
    before = (order[:, None] > order[None, :]) & (
        order[:, None] // block == order[None, :] // block
    )
    ranks = jnp.dot(
        before.astype(BF16), chosen.astype(BF16), preferred_element_type=F32
    ).astype(jnp.int32)
    base = (order // block)[:, None] * slot_cap + jnp.arange(ep, dtype=jnp.int32)[None, :] * slots
    place = jnp.where(chosen, base + ranks, -1)

    vmem = pl.BlockSpec(memory_space=pltpu.VMEM)
    anywhere = pl.BlockSpec(memory_space=pl.ANY)
    dma = pltpu.SemaphoreType.DMA
    return pl.pallas_call(
        functools.partial(layer_kernel, (ep, tp, rows, slots, feat, chunks, cols)),
        out_shape=jax.ShapeDtypeStruct((block, width), BF16),
        in_specs=[vmem] * 8 + [anywhere] * 4,
        out_specs=vmem,
        scratch_shapes=[
            pltpu.VMEM((width, hid), BF16),
            pltpu.VMEM((width, hid), BF16),
            pltpu.VMEM((hid, width), BF16),
            pltpu.VMEM((shared_rows, width), BF16),
            pltpu.VMEM((tp, rows, feat), BF16),
            pltpu.VMEM((ep, slots, rows), BF16),
            pltpu.VMEM((rows, ep * slots), BF16),
            pltpu.VMEM((tp, ep, slots, feat), BF16),
            pltpu.VMEM((tp, ep, slots, feat), BF16),
            pltpu.VMEM((max(rows, slots), width), BF16),
            pltpu.VMEM((ep, slots, hid), BF16),
            pltpu.VMEM((rows, shared_rows), BF16),
            pltpu.VMEM((chunks, ep, slots, cols), BF16),
            pltpu.VMEM((chunks, ep, slots, cols), BF16),
            pltpu.VMEM((tp, block, cols), F32),
            pltpu.VMEM((chunks, block, cols), F32),
            pltpu.VMEM((chunks, chips, block, cols), BF16),
            pltpu.VMEM((chunks, chips, block, cols), BF16),
            pltpu.VMEM((chunks, chips, block, cols), BF16),
            pltpu.VMEM((chunks, chips, block, cols), BF16),
            dma((4,)),
            dma((chips,)),
            dma((chips,)),
            dma((tp,)),
            dma((tp, ep)),
            dma((tp, ep)),
            dma((chunks, ep)),
            dma((chunks, ep)),
            dma((chunks,)),
            dma((chunks,)),
            dma((chunks, chips)),
            dma((chunks, chips)),
        ],
        compiler_params=pltpu.CompilerParams(
            collective_id=0, has_side_effects=True, vmem_limit_bytes=56 * 1024 * 1024
        ),
        name="moe_layer",
    )(
        tokens,
        place,
        place.T,
        pair_weight,
        norm_gain.reshape(1, width),
        norm_shift.reshape(1, width),
        shared_gate,
        shared_up,
        expert_gate[0],
        expert_up[0],
        expert_down[0],
        shared_down,
    )


def solution(mesh):
    placed = (
        P("ep", "tp"),
        P(),
        P(),
        P("ep", None),
        P("ep", None),
        P(("ep", "tp"), None, None),
        P(("ep", "tp"), None, None),
        P(("ep", "tp"), None, None),
        P("tp", None),
        P("tp", None),
        P(),
    )
    return jax.shard_map(
        on_device, mesh=mesh, in_specs=placed, out_specs=P(("ep", "tp"), None), check_vma=False
    )
```

```python
import functools
import math

import jax
import jax.numpy as jnp
from jax import lax
from jax.experimental import pallas as pl
from jax.experimental.pallas import tpu as pltpu
from jax.sharding import PartitionSpec as P

ROUTED_SCALE = 2.5
EPSILON = 1e-05
MESH = pl.DeviceIdType.MESH
F32 = jnp.float32
BF16 = jnp.bfloat16


def partner(index, step, count):
    if count & (count - 1):
        return lax.rem(index + step, count)
    result, bit = 0, 1
    while bit < count:
        result = result + ((index // bit) % 2 + (step // bit) % 2) % 2 * bit
        bit *= 2
    return result


def layer_kernel(
    sizes,
    tokens_ref,
    ids_ref,
    affinity_ref,
    gain_ref,
    shift_ref,
    sgate_ref,
    sup_ref,
    gate_hbm,
    up_hbm,
    down_hbm,
    sdown_hbm,
    out_ref,
    gate_ref,
    up_ref,
    down_ref,
    sdown_ref,
    whole,
    pick,
    spread_t,
    spread,
    sent,
    inc,
    norm,
    hidden,
    shidden,
    res,
    ret,
    part,
    own,
    pair_out,
    pair_in,
    far_out,
    far_in,
    load_sem,
    a_send,
    f_send,
    a_recv,
    b_send,
    b_recv,
    r_send,
    r_recv,
    p_send,
    p_recv,
    q_send,
    q_recv,
):
    ep, tp, rows, slots, slot_cap, feat, chunks, cols = sizes
    chips = tp // 2
    g = lax.axis_index("ep")
    t = lax.axis_index("tp")
    z = t // 2
    c = t % 2
    mate = z * 2 + 1 - c
    width = tp * feat
    shared_rows = sdown_ref.shape[0]

    loads = [
        pltpu.make_async_copy(gate_hbm, gate_ref, load_sem.at[0]),
        pltpu.make_async_copy(up_hbm, up_ref, load_sem.at[1]),
        pltpu.make_async_copy(down_hbm, down_ref, load_sem.at[2]),
        pltpu.make_async_copy(
            sdown_hbm.at[pl.ds(pl.multiple_of(t * shared_rows, 8), shared_rows)],
            sdown_ref,
            load_sem.at[3],
        ),
    ]
    for load in loads:
        load.start()

    def remote(src, dst, send, recv, e, k):
        return pltpu.make_async_remote_copy(
            src_ref=src,
            dst_ref=dst,
            send_sem=send,
            recv_sem=recv,
            device_id=(e, k),
            device_id_type=MESH,
        )

    barrier = pltpu.get_barrier_semaphore()
    partners = [(partner(g, p, ep), t) for p in range(1, ep)]
    partners += [(g, partner(z, d, chips) * 2 + c) for d in range(1, chips)]
    partners += [(g, mate)]
    for e, k in partners:
        pl.semaphore_signal(barrier, inc=1, device_id=(e, k), device_id_type=MESH)
    ids = ids_ref[...]
    affinity = affinity_ref[...]
    weights = affinity / jnp.sum(affinity, axis=0, keepdims=True) * ROUTED_SCALE
    block = rows // tp
    early = lax.broadcasted_iota(jnp.int32, (rows, rows), 0)
    late = lax.broadcasted_iota(jnp.int32, (rows, rows), 1)
    before = jnp.where((early < late) & (early // block == late // block), 1.0, 0.0).astype(BF16)
    hits = [ids == e * tp + t for e in range(ep)]
    chosen = [jnp.sum(jnp.where(hit, 1.0, 0.0), axis=0, keepdims=True) for hit in hits]
    pad = [jnp.zeros((-ep % 16, rows), F32)] if ep % 16 else []
    ranks = jnp.dot(
        jnp.concatenate(chosen + pad, axis=0).astype(BF16), before, preferred_element_type=F32
    ).astype(jnp.int32)
    base = lax.broadcasted_iota(jnp.int32, (1, rows), 1) // block * slot_cap
    line = lax.broadcasted_iota(jnp.int32, (slots, rows), 0)
    for e in range(ep):
        place = jnp.where(chosen[e] > 0.5, base + ranks[e : e + 1, :], -1)
        weight = jnp.sum(jnp.where(hits[e], weights, 0.0), axis=0, keepdims=True)
        pick[e] = jnp.where(line == place, 1.0, 0.0).astype(BF16)
        spread_t[pl.ds(e * slots, slots), :] = jnp.where(line == place, weight, 0.0)
    pl.semaphore_wait(barrier, len(partners))

    first = []
    first.append(remote(tokens_ref, whole.at[t], f_send.at[0], a_recv.at[t], g, mate))
    for d in range(1, chips):
        there = partner(z, d, chips) * 2 + c
        first.append(remote(tokens_ref, whole.at[t], a_send.at[d], a_recv.at[t], g, there))
    for copy in first:
        copy.start()
    whole[t] = tokens_ref[...]

    def forward(k, d):
        return remote(whole.at[k], whole.at[k], f_send.at[d], a_recv.at[k], g, mate)

    def chunk_at(i):
        d = i // 2
        side = i % 2
        return d, side, partner(z, d, chips) * 2 + lax.rem(c + side, 2)

    near = [p for p in range(1, ep) if not p & (p - 1)]
    far = [p for p in range(1, ep) if p & (p - 1)]
    lag = tp // 2
    half = chunks // 2

    def send_rows(k, p):
        e = partner(g, p, ep)
        remote(sent.at[k, e], inc.at[k, g], b_send.at[k, e], b_recv.at[k, g], e, t).start()

    def chunk_step(i, carry):
        d, side, k = chunk_at(i)

        @pl.when(i > 0)
        def _():
            forward(k, d).wait_recv()

        @pl.when((i > 0) & (side == 0))
        def _():
            forward(k, d).start()

        picked = jnp.dot(
            pick[...].reshape(ep * slots, rows), whole[k], preferred_element_type=F32
        ).astype(BF16)
        sent[k] = picked.reshape(ep, slots, feat)
        inc[k, g] = sent[k, g]
        for p in near:
            send_rows(k, p)
        if far:

            @pl.when(i >= lag)
            def _():
                for p in far:
                    send_rows(chunk_at(i - lag)[2], p)

        return carry

    lax.fori_loop(0, tp, chunk_step, 0)

    def late_step(i, carry):
        for p in far:
            send_rows(chunk_at(i)[2], p)
        return carry

    if far:
        lax.fori_loop(tp - lag, tp, late_step, 0)
    spread[...] = spread_t[...].T.astype(BF16)

    def normalise(read, count):
        tile = math.gcd(64, count)

        def body(i, carry):
            at = pl.ds(pl.multiple_of(i * tile, tile), tile)
            total = jnp.zeros((tile, feat), F32)
            for k in range(tp):
                total = total + read(k, at).astype(F32)
            mean = jnp.sum(total, axis=1, keepdims=True) / width
            total = jnp.zeros((tile, feat), F32)
            for k in range(tp):
                center = read(k, at).astype(F32) - mean
                total = total + center * center
            scale = lax.rsqrt(jnp.sum(total, axis=1, keepdims=True) / width + EPSILON)
            for k in range(tp):
                lanes = slice(k * feat, (k + 1) * feat)
                value = (read(k, at).astype(F32) - mean) * scale
                value = value * gain_ref[:, lanes] + shift_ref[:, lanes]
                norm[at, lanes] = value.astype(BF16)
            return carry

        lax.fori_loop(0, count // tile, body, 0)

    normalise(lambda k, at: whole[k, at, :], rows)
    contract = (((1,), (1,)), ((), ()))
    sg = lax.dot_general(norm[...], sgate_ref[...], contract, preferred_element_type=F32)
    su = lax.dot_general(norm[...], sup_ref[...], contract, preferred_element_type=F32)
    shidden[...] = (jax.nn.silu(sg) * su).astype(BF16)

    for load in loads:
        load.wait()

    def expert_step(p, carry):
        s = partner(g, p, ep)

        @pl.when(p > 0)
        def _():
            for k in range(tp):
                remote(
                    sent.at[k, s], inc.at[k, s], b_send.at[k, s], b_recv.at[k, s], s, t
                ).wait_recv()

        normalise(lambda k, at: inc[k, s, at, :], slots)
        got = norm[0:slots, :]
        gate_act = jnp.dot(got, gate_ref[...], preferred_element_type=F32)
        up_act = jnp.dot(got, up_ref[...], preferred_element_type=F32)
        hidden[s] = (jax.nn.silu(gate_act) * up_act).astype(BF16)

        @pl.when(p == 0)
        def _():
            def own_step(i, carry):
                ret[i, g] = down_rows(i, g)
                return carry

            lax.fori_loop(0, chunks, own_step, 0)

        is_near = functools.reduce(jnp.logical_or, [p == n for n in near])

        @pl.when(is_near)
        def _():
            def near_step(i, carry):
                send_result(i, s)
                return carry

            lax.fori_loop(0, half, near_step, 0)

        return carry

    def lanes_of(i):
        return pl.ds(pl.multiple_of(i * cols, cols), cols)

    def down_rows(i, s):
        return jnp.dot(
            hidden[s], down_ref[:, lanes_of(i)], preferred_element_type=F32
        ).astype(BF16)

    def send_result(i, s):
        res[i, s] = down_rows(i, s)
        remote(res.at[i, s], ret.at[i, g], r_send.at[i, s], r_recv.at[i, g], s, t).start()

    lax.fori_loop(0, ep, expert_step, 0)

    def down_step(i, carry):
        for p in far:
            send_result(i, partner(g, p, ep))

        @pl.when(i < chunks - half)
        def _():
            for p in near:
                send_result(i + half, partner(g, p, ep))

        return carry

    lax.fori_loop(0, chunks, down_step, 0)

    def pair_copy(i):
        return remote(pair_out.at[i], pair_in.at[i], p_send.at[i], p_recv.at[i], g, mate)

    def produce(i):
        for p in range(1, ep):
            s = partner(g, p, ep)
            remote(
                res.at[i, s], ret.at[i, s], r_send.at[i, s], r_recv.at[i, s], s, t
            ).wait_recv()
        total = jnp.dot(
            spread[...], ret[i].reshape(ep * slots, cols), preferred_element_type=F32
        ) + jnp.dot(shidden[...], sdown_ref[:, lanes_of(i)], preferred_element_type=F32)
        part[i % 2] = total.reshape(part.shape[1:])
        for zz in range(chips):
            pair_out[i, zz] = part[i % 2, zz * 2 + 1 - c].astype(BF16)
        pair_copy(i).start()

    def finish(i):
        pair_copy(i).wait_recv()
        for d in range(1, chips):
            zz = partner(z, d, chips)
            far_out[i, zz] = (part[i % 2, zz * 2 + c] + pair_in[i, zz].astype(F32)).astype(BF16)
            remote(
                far_out.at[i, zz],
                far_in.at[i, z],
                q_send.at[i, zz],
                q_recv.at[i, z],
                g,
                zz * 2 + c,
            ).start()
        own[i] = part[i % 2, t] + pair_in[i, z].astype(F32)

    def sum_step(i, carry):
        @pl.when(i < chunks)
        def _():
            produce(i)

        @pl.when(i > 0)
        def _():
            finish(i - 1)

        return carry

    lax.fori_loop(0, chunks + 1, sum_step, 0)

    def out_step(i, carry):
        total = own[i]
        for d in range(1, chips):
            zz = partner(z, d, chips)
            remote(
                far_out.at[i, zz],
                far_in.at[i, zz],
                q_send.at[i, zz],
                q_recv.at[i, zz],
                g,
                zz * 2 + c,
            ).wait()
            total = total + far_in[i, zz].astype(F32)
        out_ref[:, lanes_of(i)] = total.astype(BF16)
        pair_copy(i).wait_send()
        for p in range(1, ep):
            e = partner(g, p, ep)
            remote(
                res.at[i, e], ret.at[i, e], r_send.at[i, e], r_recv.at[i, e], e, t
            ).wait_send()
        return carry

    lax.fori_loop(0, chunks, out_step, 0)

    for copy in first:
        copy.wait_send()
    for d in range(1, chips):
        k = partner(z, d, chips) * 2 + c
        forward(k, d).wait_send()

    def drain(k, carry):
        for p in range(1, ep):
            e = partner(g, p, ep)
            remote(
                sent.at[k, e], inc.at[k, e], b_send.at[k, e], b_recv.at[k, e], e, t
            ).wait_send()
        return carry

    lax.fori_loop(0, tp, drain, 0)


def on_device(
    tokens,
    norm_gain,
    norm_shift,
    expert_ids,
    affinity,
    expert_gate,
    expert_up,
    expert_down,
    shared_gate,
    shared_up,
    shared_down,
):
    ep = lax.axis_size("ep")
    tp = lax.axis_size("tp")
    rows, feat = tokens.shape
    width = feat * tp
    top_count = expert_ids.shape[1]
    block = rows // tp
    expert_count = ep * tp
    slot_cap = max(1, 2 * block * top_count // expert_count)
    slots = tp * slot_cap
    hid = expert_gate.shape[2]
    shared_rows = shared_gate.shape[0]
    cols = 256
    chunks = width // cols
    chips = tp // 2

    vmem = pl.BlockSpec(memory_space=pltpu.VMEM)
    anywhere = pl.BlockSpec(memory_space=pl.ANY)
    dma = pltpu.SemaphoreType.DMA
    return pl.pallas_call(
        functools.partial(layer_kernel, (ep, tp, rows, slots, slot_cap, feat, chunks, cols)),
        out_shape=jax.ShapeDtypeStruct((block, width), BF16),
        in_specs=[vmem] * 7 + [anywhere] * 4,
        out_specs=vmem,
        scratch_shapes=[
            pltpu.VMEM((width, hid), BF16),
            pltpu.VMEM((width, hid), BF16),
            pltpu.VMEM((hid, width), BF16),
            pltpu.VMEM((shared_rows, width), BF16),
            pltpu.VMEM((tp, rows, feat), BF16),
            pltpu.VMEM((ep, slots, rows), BF16),
            pltpu.VMEM((ep * slots, rows), F32),
            pltpu.VMEM((rows, ep * slots), BF16),
            pltpu.VMEM((tp, ep, slots, feat), BF16),
            pltpu.VMEM((tp, ep, slots, feat), BF16),
            pltpu.VMEM((max(rows, slots), width), BF16),
            pltpu.VMEM((ep, slots, hid), BF16),
            pltpu.VMEM((rows, shared_rows), BF16),
            pltpu.VMEM((chunks, ep, slots, cols), BF16),
            pltpu.VMEM((chunks, ep, slots, cols), BF16),
            pltpu.VMEM((2, tp, block, cols), F32),
            pltpu.VMEM((chunks, block, cols), F32),
            pltpu.VMEM((chunks, chips, block, cols), BF16),
            pltpu.VMEM((chunks, chips, block, cols), BF16),
            pltpu.VMEM((chunks, chips, block, cols), BF16),
            pltpu.VMEM((chunks, chips, block, cols), BF16),
            dma((4,)),
            dma((chips,)),
            dma((chips,)),
            dma((tp,)),
            dma((tp, ep)),
            dma((tp, ep)),
            dma((chunks, ep)),
            dma((chunks, ep)),
            dma((chunks,)),
            dma((chunks,)),
            dma((chunks, chips)),
            dma((chunks, chips)),
        ],
        compiler_params=pltpu.CompilerParams(
            collective_id=0, has_side_effects=True, vmem_limit_bytes=56 * 1024 * 1024
        ),
        name="moe_layer",
    )(
        tokens,
        expert_ids.T,
        affinity.T,
        norm_gain.reshape(1, width),
        norm_shift.reshape(1, width),
        shared_gate,
        shared_up,
        expert_gate[0],
        expert_up[0],
        expert_down[0],
        shared_down,
    )


def solution(mesh):
    placed = (
        P("ep", "tp"),
        P(),
        P(),
        P("ep", None),
        P("ep", None),
        P(("ep", "tp"), None, None),
        P(("ep", "tp"), None, None),
        P(("ep", "tp"), None, None),
        P("tp", None),
        P("tp", None),
        P(),
    )
    return jax.shard_map(
        on_device, mesh=mesh, in_specs=placed, out_specs=P(("ep", "tp"), None), check_vma=False
    )
```

```python
import functools
import math

import jax
import jax.numpy as jnp
from jax import lax
from jax.experimental import pallas as pl
from jax.experimental.pallas import tpu as pltpu
from jax.sharding import PartitionSpec as P

ROUTED_SCALE = 2.5
EPSILON = 1e-05
MESH = pl.DeviceIdType.MESH
F32 = jnp.float32
BF16 = jnp.bfloat16


def partner(index, step, count):
    if count & (count - 1):
        return lax.rem(index + step, count)
    result, bit = 0, 1
    while bit < count:
        result = result + ((index // bit) % 2 + (step // bit) % 2) % 2 * bit
        bit *= 2
    return result


def layer_kernel(
    sizes,
    tokens_ref,
    ids_ref,
    affinity_ref,
    gain_ref,
    shift_ref,
    sgate_ref,
    sup_ref,
    gate_hbm,
    up_hbm,
    down_hbm,
    sdown_hbm,
    out_ref,
    gate_ref,
    up_ref,
    down_ref,
    sdown_ref,
    whole,
    pick,
    spread_t,
    spread,
    sent,
    inc,
    norm,
    hidden,
    shidden,
    res,
    ret,
    part,
    own,
    pair_out,
    pair_in,
    far_out,
    far_in,
    load_sem,
    a_send,
    f_send,
    a_recv,
    b_send,
    b_recv,
    r_send,
    r_recv,
    p_send,
    p_recv,
    q_send,
    q_recv,
):
    ep, tp, rows, slots, slot_cap, feat, chunks, cols = sizes
    chips = tp // 2
    g = lax.axis_index("ep")
    t = lax.axis_index("tp")
    z = t // 2
    c = t % 2
    mate = z * 2 + 1 - c
    width = tp * feat
    shared_rows = sdown_ref.shape[0]

    loads = [
        pltpu.make_async_copy(gate_hbm, gate_ref, load_sem.at[0]),
        pltpu.make_async_copy(up_hbm, up_ref, load_sem.at[1]),
        pltpu.make_async_copy(down_hbm, down_ref, load_sem.at[2]),
        pltpu.make_async_copy(
            sdown_hbm.at[pl.ds(pl.multiple_of(t * shared_rows, 8), shared_rows)],
            sdown_ref,
            load_sem.at[3],
        ),
    ]
    for load in loads:
        load.start()

    def remote(src, dst, send, recv, e, k):
        return pltpu.make_async_remote_copy(
            src_ref=src,
            dst_ref=dst,
            send_sem=send,
            recv_sem=recv,
            device_id=(e, k),
            device_id_type=MESH,
        )

    barrier = pltpu.get_barrier_semaphore()
    partners = [(partner(g, p, ep), t) for p in range(1, ep)]
    partners += [(g, partner(z, d, chips) * 2 + c) for d in range(1, chips)]
    partners += [(g, mate)]
    for e, k in partners:
        pl.semaphore_signal(barrier, inc=1, device_id=(e, k), device_id_type=MESH)
    ids = ids_ref[...]
    affinity = affinity_ref[...]
    weights = affinity / jnp.sum(affinity, axis=0, keepdims=True) * ROUTED_SCALE
    block = rows // tp
    early = lax.broadcasted_iota(jnp.int32, (rows, rows), 0)
    late = lax.broadcasted_iota(jnp.int32, (rows, rows), 1)
    before = jnp.where((early < late) & (early // block == late // block), 1.0, 0.0).astype(BF16)
    hits = [ids == e * tp + t for e in range(ep)]
    chosen = [jnp.sum(jnp.where(hit, 1.0, 0.0), axis=0, keepdims=True) for hit in hits]
    pad = [jnp.zeros((-ep % 16, rows), F32)] if ep % 16 else []
    ranks = jnp.dot(
        jnp.concatenate(chosen + pad, axis=0).astype(BF16), before, preferred_element_type=F32
    ).astype(jnp.int32)
    base = lax.broadcasted_iota(jnp.int32, (1, rows), 1) // block * slot_cap
    line = lax.broadcasted_iota(jnp.int32, (slots, rows), 0)
    for e in range(ep):
        place = jnp.where(chosen[e] > 0.5, base + ranks[e : e + 1, :], -1)
        weight = jnp.sum(jnp.where(hits[e], weights, 0.0), axis=0, keepdims=True)
        pick[e] = jnp.where(line == place, 1.0, 0.0).astype(BF16)
        spread_t[pl.ds(e * slots, slots), :] = jnp.where(line == place, weight, 0.0)
    pl.semaphore_wait(barrier, len(partners))

    first = []
    first.append(remote(tokens_ref, whole.at[t], f_send.at[0], a_recv.at[t], g, mate))
    for d in range(1, chips):
        there = partner(z, d, chips) * 2 + c
        first.append(remote(tokens_ref, whole.at[t], a_send.at[d], a_recv.at[t], g, there))
    for copy in first:
        copy.start()
    whole[t] = tokens_ref[...]

    def forward(k, d):
        return remote(whole.at[k], whole.at[k], f_send.at[d], a_recv.at[k], g, mate)

    def chunk_at(i):
        d = i // 2
        side = i % 2
        return d, side, partner(z, d, chips) * 2 + lax.rem(c + side, 2)

    near = [p for p in range(1, ep) if not p & (p - 1)]
    far = [p for p in range(1, ep) if p & (p - 1)]
    lag = 3 * tp // 8
    half = chunks // 8

    def send_rows(k, p):
        e = partner(g, p, ep)
        remote(sent.at[k, e], inc.at[k, g], b_send, b_recv.at[g], e, t).start()

    def chunk_step(i, carry):
        d, side, k = chunk_at(i)

        @pl.when(i > 0)
        def _():
            forward(k, d).wait_recv()

        @pl.when((i > 0) & (side == 0))
        def _():
            forward(k, d).start()

        picked = jnp.dot(
            pick[...].reshape(ep * slots, rows), whole[k], preferred_element_type=F32
        ).astype(BF16)
        sent[k] = picked.reshape(ep, slots, feat)
        inc[k, g] = sent[k, g]
        for p in near:
            send_rows(k, p)
        if far:

            @pl.when(i >= lag)
            def _():
                for p in far:
                    send_rows(chunk_at(i - lag)[2], p)

        return carry

    lax.fori_loop(0, tp, chunk_step, 0)

    def late_step(i, carry):
        for p in far:
            send_rows(chunk_at(i)[2], p)
        return carry

    if far:
        lax.fori_loop(tp - lag, tp, late_step, 0)
    spread[...] = spread_t[...].T.astype(BF16)

    def normalise(read, count):
        tile = math.gcd(64, count)

        def body(i, carry):
            at = pl.ds(pl.multiple_of(i * tile, tile), tile)
            total = jnp.zeros((tile, feat), F32)
            for k in range(tp):
                total = total + read(k, at).astype(F32)
            mean = jnp.sum(total, axis=1, keepdims=True) / width
            total = jnp.zeros((tile, feat), F32)
            for k in range(tp):
                center = read(k, at).astype(F32) - mean
                total = total + center * center
            scale = lax.rsqrt(jnp.sum(total, axis=1, keepdims=True) / width + EPSILON)
            for k in range(tp):
                lanes = slice(k * feat, (k + 1) * feat)
                value = (read(k, at).astype(F32) - mean) * scale
                value = value * gain_ref[:, lanes] + shift_ref[:, lanes]
                norm[at, lanes] = value.astype(BF16)
            return carry

        lax.fori_loop(0, count // tile, body, 0)

    normalise(lambda k, at: whole[k, at, :], rows)
    contract = (((1,), (1,)), ((), ()))
    sg = lax.dot_general(norm[...], sgate_ref[...], contract, preferred_element_type=F32)
    su = lax.dot_general(norm[...], sup_ref[...], contract, preferred_element_type=F32)
    shidden[...] = (jax.nn.silu(sg) * su).astype(BF16)

    for load in loads:
        load.wait()

    def expert_step(p, carry):
        s = partner(g, p, ep)

        @pl.when(p > 0)
        def _():
            remote(sent.at[:, s], inc.at[:, s], b_send, b_recv.at[s], s, t).wait_recv()

        normalise(lambda k, at: inc[k, s, at, :], slots)
        got = norm[0:slots, :]
        gate_act = jnp.dot(got, gate_ref[...], preferred_element_type=F32)
        up_act = jnp.dot(got, up_ref[...], preferred_element_type=F32)
        hidden[s] = (jax.nn.silu(gate_act) * up_act).astype(BF16)

        @pl.when(p == 0)
        def _():
            def own_step(i, carry):
                ret[i, g] = down_rows(i, g)
                return carry

            lax.fori_loop(0, chunks, own_step, 0)

        is_near = functools.reduce(jnp.logical_or, [p == n for n in near])

        @pl.when(is_near)
        def _():
            def near_step(i, carry):
                send_result(i, s)
                return carry

            lax.fori_loop(0, half, near_step, 0)

        return carry

    def lanes_of(i):
        return pl.ds(pl.multiple_of(i * cols, cols), cols)

    def down_rows(i, s):
        return jnp.dot(
            hidden[s], down_ref[:, lanes_of(i)], preferred_element_type=F32
        ).astype(BF16)

    def send_result(i, s):
        res[i, s] = down_rows(i, s)
        remote(res.at[i, s], ret.at[i, g], r_send, r_recv.at[i], s, t).start()

    lax.fori_loop(0, ep, expert_step, 0)

    def down_step(i, carry):
        for p in far:
            send_result(i, partner(g, p, ep))

        @pl.when(i < chunks - half)
        def _():
            for p in near:
                send_result(i + half, partner(g, p, ep))

        return carry

    lax.fori_loop(0, chunks, down_step, 0)

    def pair_copy(i):
        return remote(pair_out.at[i], pair_in.at[i], p_send, p_recv.at[i], g, mate)

    def produce(i):
        others = pl.ds(0, ep - 1)
        remote(res.at[i, others], ret.at[i, others], r_send, r_recv.at[i], g, mate).wait_recv()
        total = jnp.dot(
            spread[...], ret[i].reshape(ep * slots, cols), preferred_element_type=F32
        ) + jnp.dot(shidden[...], sdown_ref[:, lanes_of(i)], preferred_element_type=F32)
        part[i % 2] = total.reshape(part.shape[1:])
        for zz in range(chips):
            pair_out[i, zz] = part[i % 2, zz * 2 + 1 - c].astype(BF16)
        pair_copy(i).start()

    def finish(i):
        pair_copy(i).wait_recv()
        for d in range(1, chips):
            zz = partner(z, d, chips)
            far_out[i, zz] = (part[i % 2, zz * 2 + c] + pair_in[i, zz].astype(F32)).astype(BF16)
            remote(
                far_out.at[i, zz],
                far_in.at[i, z],
                q_send,
                q_recv,
                g,
                zz * 2 + c,
            ).start()
        own[i] = part[i % 2, t] + pair_in[i, z].astype(F32)

    def sum_step(i, carry):
        @pl.when(i < chunks)
        def _():
            produce(i)

        @pl.when(i > 0)
        def _():
            finish(i - 1)

        return carry

    lax.fori_loop(0, chunks + 1, sum_step, 0)

    rest = pl.ds(0, chips - 1)
    remote(far_out.at[:, rest], far_in.at[:, rest], q_send, q_recv, g, mate).wait()

    def out_step(i, carry):
        total = own[i]
        for d in range(1, chips):
            total = total + far_in[i, partner(z, d, chips)].astype(F32)
        out_ref[:, lanes_of(i)] = total.astype(BF16)
        return carry

    lax.fori_loop(0, chunks, out_step, 0)

    others = pl.ds(0, ep - 1)
    remote(sent.at[:, others], inc.at[:, others], b_send, b_recv.at[g], g, mate).wait_send()
    remote(res.at[:, others], ret.at[:, others], r_send, r_recv.at[0], g, mate).wait_send()
    remote(pair_out, pair_in, p_send, p_recv.at[0], g, mate).wait_send()
    for copy in first:
        copy.wait_send()
    for d in range(1, chips):
        k = partner(z, d, chips) * 2 + c
        forward(k, d).wait_send()


def on_device(
    tokens,
    norm_gain,
    norm_shift,
    expert_ids,
    affinity,
    expert_gate,
    expert_up,
    expert_down,
    shared_gate,
    shared_up,
    shared_down,
):
    ep = lax.axis_size("ep")
    tp = lax.axis_size("tp")
    rows, feat = tokens.shape
    width = feat * tp
    top_count = expert_ids.shape[1]
    block = rows // tp
    expert_count = ep * tp
    slot_cap = max(1, 2 * block * top_count // expert_count)
    slots = tp * slot_cap
    hid = expert_gate.shape[2]
    shared_rows = shared_gate.shape[0]
    cols = 256
    chunks = width // cols
    chips = tp // 2

    vmem = pl.BlockSpec(memory_space=pltpu.VMEM)
    anywhere = pl.BlockSpec(memory_space=pl.ANY)
    dma = pltpu.SemaphoreType.DMA
    return pl.pallas_call(
        functools.partial(layer_kernel, (ep, tp, rows, slots, slot_cap, feat, chunks, cols)),
        out_shape=jax.ShapeDtypeStruct((block, width), BF16),
        in_specs=[vmem] * 7 + [anywhere] * 4,
        out_specs=vmem,
        scratch_shapes=[
            pltpu.VMEM((width, hid), BF16),
            pltpu.VMEM((width, hid), BF16),
            pltpu.VMEM((hid, width), BF16),
            pltpu.VMEM((shared_rows, width), BF16),
            pltpu.VMEM((tp, rows, feat), BF16),
            pltpu.VMEM((ep, slots, rows), BF16),
            pltpu.VMEM((ep * slots, rows), F32),
            pltpu.VMEM((rows, ep * slots), BF16),
            pltpu.VMEM((tp, ep, slots, feat), BF16),
            pltpu.VMEM((tp, ep, slots, feat), BF16),
            pltpu.VMEM((max(rows, slots), width), BF16),
            pltpu.VMEM((ep, slots, hid), BF16),
            pltpu.VMEM((rows, shared_rows), BF16),
            pltpu.VMEM((chunks, ep, slots, cols), BF16),
            pltpu.VMEM((chunks, ep, slots, cols), BF16),
            pltpu.VMEM((2, tp, block, cols), F32),
            pltpu.VMEM((chunks, block, cols), F32),
            pltpu.VMEM((chunks, chips, block, cols), BF16),
            pltpu.VMEM((chunks, chips, block, cols), BF16),
            pltpu.VMEM((chunks, chips, block, cols), BF16),
            pltpu.VMEM((chunks, chips, block, cols), BF16),
            dma((4,)),
            dma((chips,)),
            dma((chips,)),
            dma((tp,)),
            dma,
            dma((ep,)),
            dma,
            dma((chunks,)),
            dma,
            dma((chunks,)),
            dma,
            dma,
        ],
        compiler_params=pltpu.CompilerParams(
            collective_id=0, has_side_effects=True, vmem_limit_bytes=56 * 1024 * 1024
        ),
        name="moe_layer",
    )(
        tokens,
        expert_ids.T,
        affinity.T,
        norm_gain.reshape(1, width),
        norm_shift.reshape(1, width),
        shared_gate,
        shared_up,
        expert_gate[0],
        expert_up[0],
        expert_down[0],
        shared_down,
    )


def solution(mesh):
    placed = (
        P("ep", "tp"),
        P(),
        P(),
        P("ep", None),
        P("ep", None),
        P(("ep", "tp"), None, None),
        P(("ep", "tp"), None, None),
        P(("ep", "tp"), None, None),
        P("tp", None),
        P("tp", None),
        P(),
    )
    return jax.shard_map(
        on_device, mesh=mesh, in_specs=placed, out_specs=P(("ep", "tp"), None), check_vma=False
    )
```
